512 devices in a mesh: sp: 128 (over z, x, core), tp: 4 (over y).
Axes of the slice: x: 4, y: 4, z: 16, core: 2. Of those that a mesh axis runs over, the one named last changes fastest.
Arguments:
- tokens: bfloat16 [16384, 2048], P('sp'), may hold values from -6 to 6
- pre_gain: float32 [2048], replicated, may hold values from 0.1 to 1.9
- outer_gate: bfloat16 [2048, 1024], P('sp', 'tp'), may hold values from -0.125 to 0.125
- inner_gate: bfloat16 [2048, 1024], P('sp', 'tp'), may hold values from -0.125 to 0.125
- conv_input: bfloat16 [2048, 1024], P('sp', 'tp'), may hold values from -0.125 to 0.125
- conv_taps: float32 [3, 1024], P(None, 'tp'), may hold values from -3.5 to 3.5
- query_down: bfloat16 [2048, 768], P(None, 'tp'), may hold values from -0.088388348 to 0.088388348
- latent_down: bfloat16 [2048, 512], P(None, 'tp'), may hold values from -0.088388348 to 0.088388348
- rotary_down: bfloat16 [2048, 32], replicated, may hold values from -0.125 to 0.125
- query_gain: float32 [768], replicated, may hold values from 1 to 3
- latent_gain: float32 [512], replicated, may hold values from 1 to 3
- query_up: bfloat16 [768, 512], P(None, 'tp'), may hold values from -0.14433757 to 0.14433757
- query_rotary: bfloat16 [768, 256], P(None, 'tp'), may hold values from -0.21875 to 0.21875
- key_up: bfloat16 [512, 512], P(None, 'tp'), may hold values from -4.33012702 to 4.33012702
- value_up: bfloat16 [512, 512], P(None, 'tp'), may hold values from -0.25 to 0.25
- conv_output: bfloat16 [1024, 2048], P('tp'), may hold values from -0.15625 to 0.15625
- heads_output: bfloat16 [512, 2048], P('tp'), may hold values from -0.15625 to 0.15625
- post_gain: float32 [2048], replicated, may hold values from 0.1 to 1.9
Outputs:
- mixed: bfloat16 [16384, 2048], P(('sp', 'tp'))
- row_logsum: float32 [8, 16384], P('tp', 'sp')
The draws below stay inside these ranges and needn't reach their ends.
All inputs are finite; a program needn't handle non-finite values.
Results may differ from the reference program's by a relative error of at most 0.013.
Values may be sent and summed in bfloat16 or wider, within the bound.
A program may use at most 64 MiB of HBM per device.

```python
import math
import jax
import jax.numpy as jnp
from jax import lax

D = 2048
D_CONV = 1024
HEADS = 8
NOPE = 64
ROPE = 32
VDIM = 64
QLAT = 768
KVLAT = 512
TAPS = 3
TOKENS = 16384


def clipped(key, shape, fan_in):
    return jnp.clip(jax.random.normal(key, shape, jnp.float32), -3.95, 3.95) * fan_in ** (-0.5)


def shared_down(key):
    return clipped(jax.random.fold_in(key, 101), (D, QLAT), D)


def shared_up(key):
    return clipped(jax.random.fold_in(key, 103), (QLAT, HEADS * NOPE), QLAT)


def draw_query_down(key, part):
    return shared_down(key).astype(jnp.bfloat16)


def draw_latent_down(key, part):
    result = clipped(jax.random.fold_in(key, 102), (D, KVLAT), D)
    return result.astype(jnp.bfloat16)


def draw_query_up(key, part):
    return shared_up(key).astype(jnp.bfloat16)


def draw_key_up(key, part):
    result = clipped(jax.random.fold_in(key, 105), (KVLAT, HEADS * NOPE), KVLAT)
    return result.astype(jnp.bfloat16)


def block_levels(stream_key, shape, split, low, high):
    level = 1.0
    for dim, blocks in split:
        steps = jax.random.uniform(jax.random.fold_in(jax.random.fold_in(stream_key, 6), dim), (blocks,), jnp.float32, low / len(split), high / len(split))
        level = level * jnp.repeat(jnp.exp(steps), shape[dim] // blocks).reshape((-1,) + (1,) * (len(shape) - 1 - dim))
    return level


def gaussian(key, extent, spread, reach, shards=(), held_as=jnp.bfloat16):
    array = spread * jax.random.normal(key, extent, jnp.float32)
    if shards:
        array = array * block_levels(key, extent, shards, -0.22, 0.18)
    return jnp.clip(array, -reach, reach).astype(held_as)


def setup_inputs(seed: int = 0) -> dict:
    arg_keys = jax.random.split(jax.random.key(seed), 19)
    return {
        "tokens": gaussian(arg_keys[0], (TOKENS, D), 1.0, 6.0, ((0, 128),)),
        "pre_gain": jnp.clip(1.0 + 0.18 * jax.random.normal(arg_keys[1], (D,), jnp.float32), 0.1, 1.9),
        "outer_gate": gaussian(arg_keys[2], (D, D_CONV), D ** -0.5, 0.125, ((0, 128), (1, 4))),
        "inner_gate": gaussian(arg_keys[3], (D, D_CONV), D ** -0.5, 0.125, ((0, 128), (1, 4))),
        "conv_input": gaussian(arg_keys[4], (D, D_CONV), D ** -0.5, 0.125, ((0, 128), (1, 4))),
        "conv_taps": gaussian(arg_keys[5], (TAPS, D_CONV), TAPS ** -0.5, 3.5, ((1, 4),), jnp.float32),
        "query_down": draw_query_down(jax.random.fold_in(arg_keys[18], 71), 0),
        "latent_down": draw_latent_down(jax.random.fold_in(arg_keys[18], 71), 0),
        "rotary_down": gaussian(arg_keys[8], (D, ROPE), D ** -0.5, 0.125),
        "query_gain": jnp.clip(jnp.exp(jax.random.uniform(arg_keys[9], (QLAT,), jnp.float32, math.log(1.0), math.log(3.0))), 1.0, 3.0),
        "latent_gain": jnp.clip(jnp.exp(jax.random.uniform(arg_keys[10], (KVLAT,), jnp.float32, math.log(1.0), math.log(3.0))), 1.0, 3.0),
        "query_up": draw_query_up(jax.random.fold_in(arg_keys[18], 71), 0),
        "query_rotary": gaussian(arg_keys[12], (QLAT, HEADS * ROPE), QLAT ** -0.5, 0.21875, ((1, 4),)),
        "key_up": draw_key_up(jax.random.fold_in(arg_keys[18], 71), 0),
        "value_up": gaussian(arg_keys[14], (KVLAT, HEADS * VDIM), KVLAT ** -0.5, 0.25, ((1, 4),)),
        "conv_output": gaussian(arg_keys[15], (D_CONV, D), (D_CONV + HEADS * VDIM) ** -0.5, 0.15625, ((0, 4),)),
        "heads_output": gaussian(arg_keys[16], (HEADS * VDIM, D), (D_CONV + HEADS * VDIM) ** -0.5, 0.15625, ((0, 4),)),
        "post_gain": jnp.clip(1.0 + 0.18 * jax.random.normal(arg_keys[17], (D,), jnp.float32), 0.1, 1.9),
    }


eps = 1e-06
rope_theta = 500000.0

def rms_scale(values, scale_row):
    widened = values.astype(jnp.float32)
    return widened * lax.rsqrt(lax.optimization_barrier(jnp.mean(widened * widened, axis=-1, keepdims=True)) + eps) * scale_row

def rotate(values, positions):
    half_width = values.shape[-1] // 2
    frequency = rope_theta ** (-jnp.arange(half_width, dtype=jnp.float32) / half_width)
    angles = positions.astype(jnp.float32)[:, None] * frequency
    cosine = jnp.cos(angles)[:, None, :]
    sine_part = jnp.sin(angles)[:, None, :]
    leading = values[..., :half_width]
    trailing = values[..., half_width:]
    return jnp.concatenate([leading * cosine - trailing * sine_part, trailing * cosine + leading * sine_part], axis=-1)

def reference(tokens, pre_gain, outer_gate, inner_gate, conv_input, conv_taps, query_down, latent_down, rotary_down, query_gain, latent_gain, query_up, query_rotary, key_up, value_up, conv_output, heads_output, post_gain):
    normed = rms_scale(tokens, pre_gain).astype(jnp.bfloat16)
    positions = jnp.arange(TOKENS, dtype=jnp.int32)
    outer_part = jnp.dot(normed, outer_gate, preferred_element_type=jnp.float32)
    inner_part = jnp.dot(normed, inner_gate, preferred_element_type=jnp.float32)
    signal = jnp.dot(normed, conv_input, preferred_element_type=jnp.float32)
    product = (inner_part * signal).astype(jnp.bfloat16)
    extended = jnp.concatenate([jnp.zeros((TAPS - 1, D_CONV), jnp.float32), product.astype(jnp.float32)], axis=0)
    convolved = extended[0:TOKENS] * conv_taps[0]
    for offset in range(1, TAPS):
        convolved = convolved + extended[offset:offset + TOKENS] * conv_taps[offset]
    conv_mixed = (outer_part * convolved).astype(jnp.bfloat16)
    query_latent = jnp.dot(normed, query_down, preferred_element_type=jnp.float32).astype(jnp.bfloat16)
    key_latent = jnp.dot(normed, latent_down, preferred_element_type=jnp.float32).astype(jnp.bfloat16)
    query_normed = rms_scale(query_latent, query_gain).astype(jnp.bfloat16)
    latent_normed = rms_scale(key_latent, latent_gain).astype(jnp.bfloat16)
    rotary_raw = jnp.dot(normed, rotary_down, preferred_element_type=jnp.float32)
    key_rotary = rotate(rotary_raw[:, None, :], positions)[:, 0, :].astype(jnp.bfloat16)
    query_nope = jnp.dot(query_normed, query_up, preferred_element_type=jnp.float32).astype(jnp.bfloat16)
    query_nope = query_nope.reshape(TOKENS, HEADS, NOPE)
    turned_raw = jnp.dot(query_normed, query_rotary, preferred_element_type=jnp.float32)
    query_turned = rotate(turned_raw.reshape(TOKENS, HEADS, ROPE), positions).astype(jnp.bfloat16)
    key_nope = jnp.dot(latent_normed, key_up, preferred_element_type=jnp.float32).astype(jnp.bfloat16)
    key_nope = key_nope.reshape(TOKENS, HEADS, NOPE).astype(jnp.float32)
    value_rows = jnp.dot(latent_normed, value_up, preferred_element_type=jnp.float32).astype(jnp.bfloat16)
    value_rows = value_rows.reshape(TOKENS, HEADS, VDIM).astype(jnp.float32)
    key_wide = key_rotary.astype(jnp.float32)
    score_scale = (NOPE + ROPE) ** (-0.5)
    block_rows = 512 if TOKENS % 512 == 0 else TOKENS

    def one_block(block_index):
        first_row = block_index * block_rows
        query_block = lax.dynamic_slice_in_dim(query_nope, first_row, block_rows, 0).astype(jnp.float32)
        turned_block = lax.dynamic_slice_in_dim(query_turned, first_row, block_rows, 0).astype(jnp.float32)
        scores = jnp.einsum('qhd,khd->hqk', query_block, key_nope)
        scores = scores + jnp.einsum('qhd,kd->hqk', turned_block, key_wide)
        scores = scores * score_scale
        query_position = first_row + jnp.arange(block_rows, dtype=jnp.int32)
        causal = positions[None, :] <= query_position[:, None]
        scores = jnp.where(causal[None], scores, -1e+30)
        row_best = lax.optimization_barrier(jnp.max(scores, axis=-1))
        weights = jnp.where(causal[None], jnp.exp(scores - row_best[..., None]), 0.0)
        weight_sum = lax.optimization_barrier(jnp.sum(weights, axis=-1))
        rounded = lax.optimization_barrier(weights.astype(jnp.bfloat16))
        weighted = jnp.einsum('hqk,khd->hqd', rounded.astype(jnp.float32), value_rows)
        mixed_block = (weighted / weight_sum[..., None]).astype(jnp.bfloat16)
        return (mixed_block, row_best + jnp.log(weight_sum))
    blocks_out, logsums = lax.map(one_block, jnp.arange(TOKENS // block_rows, dtype=jnp.int32))
    heads_mixed = blocks_out.transpose(0, 2, 1, 3).reshape(TOKENS, HEADS * VDIM)
    row_logsum = logsums.transpose(1, 0, 2).reshape(HEADS, TOKENS)
    projected = jnp.dot(conv_mixed, conv_output, preferred_element_type=jnp.float32)
    projected = projected + jnp.dot(heads_mixed, heads_output, preferred_element_type=jnp.float32)
    mixed = rms_scale(projected, post_gain).astype(jnp.bfloat16)
    return (mixed, row_logsum)
```

```python
import math

import jax
import jax.numpy as jnp
import numpy as np
from jax import lax
from jax.experimental import pallas as pl
from jax.experimental.pallas import tpu as pltpu
from jax.sharding import Mesh
from jax.sharding import PartitionSpec as P

NOPE = 64
ROPE = 32
VDIM = 64
EPS = 1e-06
THETA = 500000.0
NZ, NX, NC, NY = 16, 4, 2, 4
NP = NX * NC
ROWS = 128
HEADS = 2
SLAB = NP * ROWS
UP, DOWN = NZ // 2, NZ // 2 - 1
PIECES = 3
PIECE = 96
KV_ROWS = 288
TILE = 256
AHEAD = 3
LOG2E = math.log2(math.e)
SCALE2 = (NOPE + ROPE) ** (-0.5) * LOG2E
LOW = -1e30
F32 = jnp.float32
BF16 = jnp.bfloat16
MESH = pl.DeviceIdType.MESH
SP = ("z", "x", "c")


def angle_tables():
    half = ROPE // 2
    frequency = THETA ** (-np.arange(half, dtype=np.float64) / half)
    near = np.arange(ROWS, dtype=np.float64)
    far = np.arange(NZ * NP, dtype=np.float64) * ROWS
    parts = []
    for places in (near, far):
        angles = frequency[:, None] * places[None, :]
        parts += [np.cos(angles), np.sin(angles)]
    return np.concatenate(parts, axis=0).astype(np.float32)


def dot(a, b):
    return jnp.dot(a, b, preferred_element_type=F32)


def kernel(
    tokens, pre_gain, outer_gate, inner_gate, conv_input, taps, query_down, latent_down,
    rotary_down, query_gain, latent_gain, query_up, query_rotary, key_up, value_up,
    conv_output, heads_output, post_gain, angles,
    out, logsum,
    normed, weights, latk, latq, kv, queries, blocks, acc, stats, sent_o, sent_s, got_o, got_s,
    product, sums, got_sums,
    w_got, w_sib_got, w_sent_z, w_sent_x, w_sent_f, w_sib_sent,
    kv_got, kv_sent, k_got, k_sent, q_got, q_sent, g_got, g_sent,
    o_got, o_sent, s_got, s_sent, h_got, h_sent, y_got, y_sent,
):
    z, x, c, y = (lax.axis_index(a) for a in ("z", "x", "c", "y"))
    me = x * NC + c
    zup, zdown = lax.rem(z + 1, NZ), lax.rem(z + NZ - 1, NZ)
    xright, xleft = lax.rem(x + 1, NX), lax.rem(x + NX - 1, NX)
    xfar = lax.rem(x + 2, NX)
    has_next = jnp.logical_or(me < NP - 1, z < NZ - 1)
    has_prev = jnp.logical_or(me > 0, z > 0)
    next_p = lax.rem(me + 1, NP)
    next_dev = {
        "z": jnp.minimum(z + jnp.where(me == NP - 1, 1, 0), NZ - 1),
        "x": next_p // NC,
        "c": lax.rem(next_p, NC),
    }
    prev_dev = {
        "z": jnp.maximum(z - 1, 0),
        "x": NX - 1,
        "c": NC - 1,
    }

    def slab_dev(p):
        return {"x": p // NC, "c": lax.rem(p, NC)}

    def remote(src, dst, ssem, rsem, dev):
        return pltpu.make_async_remote_copy(
            src_ref=src, dst_ref=dst, send_sem=ssem, recv_sem=rsem, device_id=dev, device_id_type=MESH
        )

    weights[z, x, c, :, 0:256] = outer_gate[...]
    weights[z, x, c, :, 256:512] = inner_gate[...]
    weights[z, x, c, :, 512:768] = conv_input[...]

    barrier = pltpu.get_barrier_semaphore()

    def greet(dev):
        pl.semaphore_signal(barrier, inc=1, device_id=dev, device_id_type=MESH)

    greet({"z": zup})
    greet({"z": zdown})
    for d in range(1, NP):
        greet(slab_dev(lax.rem(me + d, NP)))
    for d in range(1, NY):
        greet({"y": lax.rem(y + d, NY)})
    far_next = jnp.logical_and(me == NP - 1, z < NZ - 1)
    far_prev = jnp.logical_and(me == 0, z > 0)

    @pl.when(far_next)
    def _():
        greet(next_dev)

    @pl.when(far_prev)
    def _():
        greet(prev_dev)

    pl.semaphore_wait(
        barrier, 2 + NP - 1 + NY - 1 + jnp.where(far_next, 1, 0) + jnp.where(far_prev, 1, 0)
    )

    def up_origin(s):
        return lax.rem(z + NZ - s, NZ)

    def down_origin(s):
        return lax.rem(z + s, NZ)

    def w_copy(origin, column, ssem, dev):
        block = weights.at[origin, column, c]
        return remote(block, block, ssem, w_got.at[column, origin], dev)

    def w_z(way, s):
        origin = up_origin(s) if way == 0 else down_origin(s)
        return w_copy(origin, x, w_sent_z.at[way, s], {"z": zup if way == 0 else zdown})

    def w_x(way, origin):
        return w_copy(origin, x, w_sent_x.at[way, origin], {"x": xright if way == 0 else xleft})

    def w_forward(way, origin):
        column, dev = (xleft, xright) if way == 0 else (xright, xleft)
        return w_copy(origin, column, w_sent_f.at[origin], {"x": dev})

    def w_sibling(origin):
        half = weights.at[origin, :, c]
        return remote(half, half, w_sib_sent.at[origin], w_sib_got.at[origin], {"c": 1 - c})

    def w_wait(column, origin):
        w_copy(origin, column, w_sent_f.at[origin], {"x": xright}).wait_recv()

    def w_start():
        w_z(0, 0).start()
        w_z(1, 0).start()
        w_x(0, z).start()
        w_x(1, z).start()

    def w_step_z(s):
        for way, last in ((0, UP), (1, DOWN)):
            origin = up_origin(s) if way == 0 else down_origin(s)

            @pl.when(s <= last)
            def _():
                w_wait(x, origin)

                @pl.when(s < last)
                def _():
                    w_z(way, s).start()

                w_x(0, origin).start()
                w_x(1, origin).start()

    def w_each(s, act):
        act(up_origin(s))

        @pl.when(jnp.logical_and(s >= 1, s <= DOWN))
        def _():
            act(down_origin(s))

    def w_step_x(s):
        def act(origin):
            w_wait(xleft, origin)
            w_wait(xright, origin)
            even = lax.rem(origin, 2) == 0

            @pl.when(even)
            def _():
                w_forward(0, origin).start()

            @pl.when(jnp.logical_not(even))
            def _():
                w_forward(1, origin).start()

        w_each(s, act)

    def w_step_sibling(s):
        def act(origin):
            w_wait(xfar, origin)
            w_sibling(origin).start()

        w_each(s, act)

    w_start()

    wide = tokens[...].astype(F32)
    scaled = wide * lax.rsqrt(jnp.mean(wide * wide, axis=-1, keepdims=True) + EPS) * pre_gain[...]
    normed[...] = scaled.astype(BF16)

    latk[y] = dot(normed[...], latent_down[...]).astype(BF16)

    def k_copy(d):
        return remote(latk.at[y], latk.at[y], k_sent.at[d], k_got.at[y], {"y": lax.rem(y + d, NY)})

    def k_arrival(d):
        other = lax.rem(y + d, NY)
        return remote(latk.at[other], latk.at[other], k_sent.at[d], k_got.at[other], {"y": other})

    def q_copy(d):
        return remote(latq.at[y], latq.at[y], q_sent.at[d], q_got.at[y], {"y": lax.rem(y + d, NY)})

    def q_arrival(d):
        other = lax.rem(y + d, NY)
        return remote(latq.at[other], latq.at[other], q_sent.at[d], q_got.at[other], {"y": other})

    for d in range(1, NY):
        k_copy(d).start()
    latq[y] = dot(normed[...], query_down[...]).astype(BF16)
    for d in range(1, NY):
        q_copy(d).start()

    lane = lax.broadcasted_iota(jnp.int32, (ROPE // 2, ROWS), 1)
    mine = lane == z * NP + me

    def far_value(rows):
        return jnp.sum(jnp.where(mine, rows, 0.0), axis=1, keepdims=True)

    cos_near, sin_near = angles[0:16, :], angles[16:32, :]
    cos_far, sin_far = far_value(angles[32:48, :]), far_value(angles[48:64, :])
    cosine = cos_near * cos_far - sin_near * sin_far
    sine = sin_near * cos_far + cos_near * sin_far

    def rotated(turned):
        lead, trail = turned[0:16, :], turned[16:32, :]
        return jnp.concatenate([lead * cosine - trail * sine, trail * cosine + lead * sine], axis=0)

    key_rotary = rotated(dot(normed[...], rotary_down[...]).T).astype(BF16)
    w_step_z(jnp.int32(1))

    for d in range(1, NY):
        k_arrival(d).wait_recv()
    latent = jnp.concatenate([latk[i] for i in range(NY)], axis=1).astype(F32)
    latent = latent * lax.rsqrt(jnp.mean(latent * latent, axis=-1, keepdims=True) + EPS)
    latent = (latent * latent_gain[...]).astype(BF16)
    kv[z, 0:128, :] = dot(latent, key_up[...]).astype(BF16)
    kv[z, 128:256, :] = dot(latent, value_up[...]).T.astype(BF16)
    kv[z, 256:288, :] = key_rotary

    def kv_copy(way, s, piece):
        origin = up_origin(s) if way == 0 else down_origin(s)
        rows = kv.at[origin, pl.ds(pl.multiple_of(piece * PIECE, PIECE), PIECE)]
        return remote(
            rows, rows, kv_sent.at[way, s, piece], kv_got.at[origin, piece],
            {"z": zup if way == 0 else zdown},
        )

    def kv_sends(way, s):
        if way == 0:
            return jnp.logical_and(s < UP, jnp.logical_and(z - s >= 0, z < NZ - 1))
        return jnp.logical_and(s < DOWN, down_origin(s) < DOWN)

    def kv_comes(way, s):
        if way == 0:
            return z - s >= 0
        return jnp.logical_and(s <= DOWN, down_origin(s) < DOWN)

    for way in range(2):

        @pl.when(kv_sends(way, 0))
        def _():
            for piece in range(PIECES):
                kv_copy(way, 0, piece).start()

    for d in range(1, NY):
        q_arrival(d).wait_recv()
    parts = [latq[i].astype(F32) for i in range(NY)]
    square = sum(jnp.sum(p * p, axis=-1, keepdims=True) for p in parts)
    factor = lax.rsqrt(square * (1.0 / (NY * parts[0].shape[1])) + EPS)
    nope, turned = None, None
    for i in range(NY):
        part = (parts[i] * factor * query_gain[i : i + 1, :]).astype(BF16)
        rows = slice(i * part.shape[1], (i + 1) * part.shape[1])
        a, b = dot(part, query_up[rows, :]), dot(part, query_rotary[rows, :])
        nope = a if nope is None else nope + a
        turned = b if turned is None else turned + b
    turned = turned.T
    queries[me, 0:128, :] = nope.T.astype(BF16)
    queries[me, 128:160, :] = rotated(turned[0:32, :]).astype(BF16)
    queries[me, 160:192, :] = rotated(turned[32:64, :]).astype(BF16)

    def g_copy(d):
        return remote(
            queries.at[me], queries.at[me], g_sent.at[d], g_got.at[me], slab_dev(lax.rem(me + d, NP))
        )

    def g_arrival(d):
        other = lax.rem(me + d, NP)
        return remote(queries.at[other], queries.at[other], g_sent.at[d], g_got.at[other], slab_dev(other))

    for d in range(1, NP):
        g_copy(d).start()

    w_step_x(jnp.int32(0))
    w_step_z(jnp.int32(2))
    w_step_x(jnp.int32(1))
    w_step_sibling(jnp.int32(0))
    w_step_z(jnp.int32(3))

    acc[...] = jnp.zeros_like(acc)
    stats[0:HEADS, :] = jnp.full((HEADS, SLAB), LOW, F32)
    stats[HEADS : 2 * HEADS, :] = jnp.zeros((HEADS, SLAB), F32)
    for d in range(1, NP):
        g_arrival(d).wait_recv()
    blocks[...] = jnp.zeros_like(blocks)
    for p in range(NP):
        for h in range(HEADS):
            columns = slice(h * SLAB + p * ROWS, h * SLAB + (p + 1) * ROWS)
            blocks[h * NOPE : (h + 1) * NOPE, columns] = queries[p, h * NOPE : (h + 1) * NOPE, :]
            blocks[128:160, columns] = queries[p, 128 + h * ROPE : 128 + (h + 1) * ROPE, :]

    def attend(origin, diagonal):
        keys = kv[origin, 0:128, :]
        rotary = kv[origin, 256:288, :].astype(F32).T.astype(BF16)
        keys = jnp.concatenate([keys, rotary], axis=1)
        for h in range(HEADS):
            values = kv[origin, 128 + h * VDIM : 128 + (h + 1) * VDIM, :]
            for t in range(SLAB // TILE):
                at = slice(t * TILE, (t + 1) * TILE)
                scores = dot(keys, blocks[:, h * SLAB + t * TILE : h * SLAB + (t + 1) * TILE]) * SCALE2
                if diagonal:
                    key = me * ROWS + lax.broadcasted_iota(jnp.int32, (ROWS, TILE), 0)
                    query = t * TILE + lax.broadcasted_iota(jnp.int32, (ROWS, TILE), 1)
                    seen = key <= query
                    scores = jnp.where(seen, scores, LOW)
                old = stats[h : h + 1, at]
                best = jnp.maximum(old, jnp.max(scores, axis=0, keepdims=True))
                weight = jnp.exp2(scores - best)
                if diagonal:
                    weight = jnp.where(seen, weight, 0.0)
                shrink = jnp.exp2(old - best)
                stats[h : h + 1, at] = best
                total = slice(HEADS + h, HEADS + h + 1)
                stats[total, at] = stats[total, at] * shrink + jnp.sum(weight, axis=0, keepdims=True)
                acc[h, :, at] = acc[h, :, at] * shrink + dot(values, weight.astype(BF16))

    attend(z, True)

    def ring_step(s, carry):
        for piece in range(PIECES):
            for way in range(2):

                @pl.when(kv_comes(way, s))
                def _():
                    origin = up_origin(s) if way == 0 else down_origin(s)
                    rows = kv.at[origin, pl.ds(piece * PIECE, PIECE)]
                    remote(
                        rows, rows, kv_sent.at[way, 0, piece], kv_got.at[origin, piece], {"z": zup}
                    ).wait_recv()

                    @pl.when(kv_sends(way, s))
                    def _():
                        kv_copy(way, s, piece).start()

        w_step_z(s + AHEAD)

        @pl.when(s + 1 <= UP)
        def _():
            w_step_x(s + 1)

        w_step_sibling(s)

        @pl.when(z - s >= 0)
        def _():
            attend(up_origin(s), False)

        @pl.when(jnp.logical_and(s <= DOWN, z + s >= NZ))
        def _():
            attend(down_origin(s), False)

        return carry

    lax.fori_loop(1, UP + 1, ring_step, jnp.int32(0))

    for p in range(NP):
        at = slice(p * ROWS, (p + 1) * ROWS)
        for h in range(HEADS):
            sent_o[p, h * VDIM : (h + 1) * VDIM, :] = acc[h, :, at].astype(BF16)
        sent_s[p, 0 : 2 * HEADS, :] = stats[:, at]
        sent_s[p, 2 * HEADS : 8, :] = jnp.zeros((8 - 2 * HEADS, ROWS), F32)

    def o_copy(d):
        p = lax.rem(me + d, NP)
        return remote(sent_o.at[p], got_o.at[me], o_sent.at[d], o_got.at[me], slab_dev(p))

    def s_copy(d):
        p = lax.rem(me + d, NP)
        return remote(sent_s.at[p], got_s.at[me], s_sent.at[d], s_got.at[me], slab_dev(p))

    def o_arrival(d):
        p = lax.rem(me + d, NP)
        return remote(sent_o.at[p], got_o.at[p], o_sent.at[d], o_got.at[p], slab_dev(p))

    def s_arrival(d):
        p = lax.rem(me + d, NP)
        return remote(sent_s.at[p], got_s.at[p], s_sent.at[d], s_got.at[p], slab_dev(p))

    for d in range(1, NP):
        o_copy(d).start()
        s_copy(d).start()
    got_o[me] = sent_o[me]
    got_s[me] = sent_s[me]

    mixed_in = None
    for k in range(NZ // 2):
        for i in range(2):
            half = weights.at[2 * k + i, :, 1 - c]
            remote(
                half, half, w_sib_sent.at[2 * k + i], w_sib_got.at[2 * k + i], {"c": 1 - c}
            ).wait_recv()
        part = dot(
            normed[:, 256 * k : 256 * (k + 1)],
            weights[2 * k : 2 * k + 2].reshape(256, 768),
        )
        mixed_in = part if mixed_in is None else mixed_in + part
    outer_part = mixed_in[:, 0:256]
    product[16:144, :] = (mixed_in[:, 256:512] * mixed_in[:, 512:768]).astype(BF16)

    h_copy = remote(product.at[pl.ds(128, 16)], product.at[pl.ds(0, 16)], h_sent, h_got, next_dev)

    @pl.when(has_next)
    def _():
        h_copy.start()

    @pl.when(has_prev)
    def _():
        h_copy.wait_recv()

    @pl.when(jnp.logical_not(has_prev))
    def _():
        product[0:16, :] = jnp.zeros((16, 256), BF16)

    extended = product[...].astype(F32)
    convolved = pltpu.roll(extended, 2, axis=0)[16:144] * taps[0:1, :]
    convolved = convolved + pltpu.roll(extended, 1, axis=0)[16:144] * taps[1:2, :]
    convolved = convolved + extended[16:144] * taps[2:3, :]
    conv_mixed = (outer_part * convolved).astype(BF16)

    for d in range(1, NP):
        o_arrival(d).wait_recv()
        s_arrival(d).wait_recv()
    heads = []
    for h in range(HEADS):
        best = got_s[0, h : h + 1, :]
        for p in range(1, NP):
            best = jnp.maximum(best, got_s[p, h : h + 1, :])
        total, weighted = None, None
        for p in range(NP):
            factor = jnp.exp2(got_s[p, h : h + 1, :] - best)
            a = got_s[p, HEADS + h : HEADS + h + 1, :] * factor
            b = got_o[p, h * VDIM : (h + 1) * VDIM, :].astype(F32) * factor
            total = a if total is None else total + a
            weighted = b if weighted is None else weighted + b
        logsum[h : h + 1, :] = (best + jnp.log2(total)) * (1.0 / LOG2E)
        heads.append(weighted / total)
    heads_mixed = jnp.concatenate(heads, axis=0).T.astype(BF16)

    quarter = ROWS // NY

    def y_copy(d):
        p = lax.rem(y + d, NY)
        return remote(sums.at[p], got_sums.at[y], y_sent.at[d], y_got.at[y], {"y": p})

    def y_arrival(d):
        p = lax.rem(y + d, NY)
        return remote(sums.at[p], got_sums.at[p], y_sent.at[d], y_got.at[p], {"y": p})

    for t in range(4):
        at = slice(t * 512, (t + 1) * 512)
        projected = dot(conv_mixed, conv_output[:, at]) + dot(heads_mixed, heads_output[:, at])
        for p in range(NY):
            sums[p, :, at] = projected[p * quarter : (p + 1) * quarter, :].astype(BF16)
    for d in range(1, NY):
        y_copy(d).start()
    whole = sums[y].astype(F32)
    for d in range(1, NY):
        y_arrival(d).wait_recv()
        whole = whole + got_sums[lax.rem(y + d, NY)].astype(F32)
    whole = whole * lax.rsqrt(jnp.mean(whole * whole, axis=-1, keepdims=True) + EPS) * post_gain[...]
    out[...] = whole.astype(BF16)

    for d in range(1, NY):
        k_copy(d).wait_send()
        q_copy(d).wait_send()
        y_copy(d).wait_send()
    for d in range(1, NP):
        g_copy(d).wait_send()
        o_copy(d).wait_send()
        s_copy(d).wait_send()

    @pl.when(has_next)
    def _():
        h_copy.wait_send()

    def left(s, carry):
        @pl.when(s < UP)
        def _():
            w_z(0, s).wait_send()

        @pl.when(s < DOWN)
        def _():
            w_z(1, s).wait_send()

        w_x(0, s).wait_send()
        w_x(1, s).wait_send()
        w_forward(0, s).wait_send()
        w_sibling(s).wait_send()
        for way in range(2):

            @pl.when(kv_sends(way, s))
            def _():
                for piece in range(PIECES):
                    kv_copy(way, s, piece).wait_send()

        return carry

    lax.fori_loop(0, NZ, left, jnp.int32(0))


def local(
    tokens, pre_gain, outer_gate, inner_gate, conv_input, conv_taps, query_down, latent_down,
    rotary_down, query_gain, latent_gain, query_up, query_rotary, key_up, value_up,
    conv_output, heads_output, post_gain,
):
    width = tokens.shape[1]
    vmem = pl.BlockSpec(memory_space=pltpu.VMEM)
    dma = pltpu.SemaphoreType.DMA
    scratch = [
        pltpu.VMEM((ROWS, width), BF16),
        pltpu.VMEM((NZ, NX, NC, 16, 768), BF16),
        pltpu.VMEM((NY, ROWS, 128), BF16),
        pltpu.VMEM((NY, ROWS, 192), BF16),
        pltpu.VMEM((NZ, KV_ROWS, ROWS), BF16),
        pltpu.VMEM((NP, 192, ROWS), BF16),
        pltpu.VMEM((160, HEADS * SLAB), BF16),
        pltpu.VMEM((HEADS, VDIM, SLAB), F32),
        pltpu.VMEM((2 * HEADS, SLAB), F32),
        pltpu.VMEM((NP, HEADS * VDIM, ROWS), BF16),
        pltpu.VMEM((NP, 8, ROWS), F32),
        pltpu.VMEM((NP, HEADS * VDIM, ROWS), BF16),
        pltpu.VMEM((NP, 8, ROWS), F32),
        pltpu.VMEM((16 + ROWS, 256), BF16),
        pltpu.VMEM((NY, ROWS // NY, width), BF16),
        pltpu.VMEM((NY, ROWS // NY, width), BF16),
        dma((NX, NZ)),
        dma((NZ,)),
        dma((2, UP)),
        dma((2, NZ)),
        dma((NZ,)),
        dma((NZ,)),
        dma((NZ, PIECES)),
        dma((2, UP, PIECES)),
        dma((NY,)),
        dma((NY,)),
        dma((NY,)),
        dma((NY,)),
        dma((NP,)),
        dma((NP,)),
        dma((NP,)),
        dma((NP,)),
        dma((NP,)),
        dma((NP,)),
        dma,
        dma,
        dma((NY,)),
        dma((NY,)),
    ]
    return pl.pallas_call(
        kernel,
        out_shape=(
            jax.ShapeDtypeStruct((ROWS // NY, width), BF16),
            jax.ShapeDtypeStruct((HEADS, ROWS), F32),
        ),
        in_specs=[vmem] * 19,
        out_specs=(vmem, vmem),
        scratch_shapes=scratch,
        compiler_params=pltpu.CompilerParams(
            collective_id=0, has_side_effects=True, vmem_limit_bytes=48 * 1024 * 1024
        ),
        name="layer",
    )(
        tokens, pre_gain.reshape(1, -1), outer_gate, inner_gate, conv_input, conv_taps, query_down,
        latent_down, rotary_down, query_gain.reshape(NY, -1), latent_gain.reshape(1, -1), query_up,
        query_rotary, key_up, value_up, conv_output, heads_output, post_gain.reshape(1, -1),
        jnp.asarray(angle_tables()),
    )


def solution(mesh):
    split = Mesh(mesh.devices.reshape(NZ, NX, NC, NY), ("z", "x", "c", "y"))
    return jax.shard_map(
        local,
        mesh=split,
        in_specs=(
            P(SP, None), P(), P(SP, "y"), P(SP, "y"), P(SP, "y"), P(None, "y"), P(None, "y"),
            P(None, "y"), P(), P(), P(), P(None, "y"), P(None, "y"), P(None, "y"), P(None, "y"),
            P("y", None), P("y", None), P(),
        ),
        out_specs=(P(("z", "x", "c", "y"), None), P("y", SP)),
        check_vma=False,
    )
```

```python
import math

import jax
import jax.numpy as jnp
import numpy as np
from jax import lax
from jax.experimental import pallas as pl
from jax.experimental.pallas import tpu as pltpu
from jax.sharding import Mesh
from jax.sharding import PartitionSpec as P

NOPE = 64
ROPE = 32
VDIM = 64
EPS = 1e-06
THETA = 500000.0
NZ, NX, NC, NY = 16, 4, 2, 4
NP = NX * NC
ROWS = 128
HEADS = 2
SLAB = NP * ROWS
UP, DOWN = NZ // 2, NZ // 2 - 1
PIECES = 3
PIECE = 96
KV_ROWS = 288
TILE = 256
AHEAD = 3
LOG2E = math.log2(math.e)
SCALE2 = (NOPE + ROPE) ** (-0.5) * LOG2E
LOW = -1e30
F32 = jnp.float32
BF16 = jnp.bfloat16
MESH = pl.DeviceIdType.MESH
SP = ("z", "x", "c")


def angle_tables():
    half = ROPE // 2
    frequency = THETA ** (-np.arange(half, dtype=np.float64) / half)
    near = np.arange(ROWS, dtype=np.float64)
    far = np.arange(NZ * NP, dtype=np.float64) * ROWS
    parts = []
    for places in (near, far):
        angles = frequency[:, None] * places[None, :]
        parts += [np.cos(angles), np.sin(angles)]
    return np.concatenate(parts, axis=0).astype(np.float32)


def dot(a, b):
    return jnp.dot(a, b, preferred_element_type=F32)


def kernel(
    tokens_h, pre_gain_h, outer_gate_h, inner_gate_h, conv_input_h, taps_h, query_down_h, latent_down_h,
    rotary_down_h, query_gain_h, latent_gain_h, query_up_h, query_rotary_h, key_up_h, value_up_h,
    conv_output_h, heads_output_h, post_gain_h, angles_h,
    out, logsum,
    tokens, pre_gain, taps, down, latent_down, query_gain, latent_gain, query_up, query_rotary,
    key_up, value_up, conv_output, heads_output, post_gain, angles, up_turned, gain_turned, loaded,
    normed, weights, latk, latq, kv, queries, blocks, acc, stats, sent_o, sent_s, got_o, got_s,
    product, sums, got_sums,
    w_got, w_sib_got, w_sent_z, w_sent_x, w_sent_f, w_sib_sent,
    kv_got, kv_sent, k_got, k_sent, q_got, q_sent, g_got, g_sent,
    o_got, o_sent, s_got, s_sent, h_got, h_sent, y_got, y_sent,
):
    z, x, c, y = (lax.axis_index(a) for a in ("z", "x", "c", "y"))
    me = x * NC + c
    zup, zdown = lax.rem(z + 1, NZ), lax.rem(z + NZ - 1, NZ)
    xright, xleft = lax.rem(x + 1, NX), lax.rem(x + NX - 1, NX)
    xfar = lax.rem(x + 2, NX)
    has_next = jnp.logical_or(me < NP - 1, z < NZ - 1)
    has_prev = jnp.logical_or(me > 0, z > 0)
    next_p = lax.rem(me + 1, NP)
    next_dev = {
        "z": jnp.minimum(z + jnp.where(me == NP - 1, 1, 0), NZ - 1),
        "x": next_p // NC,
        "c": lax.rem(next_p, NC),
    }
    prev_dev = {
        "z": jnp.maximum(z - 1, 0),
        "x": NX - 1,
        "c": NC - 1,
    }

    def slab_dev(p):
        return {"x": p // NC, "c": lax.rem(p, NC)}

    def remote(src, dst, ssem, rsem, dev):
        return pltpu.make_async_remote_copy(
            src_ref=src, dst_ref=dst, send_sem=ssem, recv_sem=rsem, device_id=dev, device_id_type=MESH
        )

    own = weights.at[z, x, c]
    loads = [
        pltpu.make_async_copy(src, dst, loaded.at[i])
        for i, (src, dst) in enumerate((
            (outer_gate_h, own.at[:, 0:256]),
            (inner_gate_h, own.at[:, 256:512]),
            (conv_input_h, own.at[:, 512:768]),
            (tokens_h, tokens),
            (pre_gain_h, pre_gain),
            (latent_down_h, latent_down),
            (query_down_h, down.at[0:192]),
            (rotary_down_h, down.at[192:224]),
            (angles_h, angles),
            (query_up_h, query_up),
            (latent_gain_h, latent_gain),
            (key_up_h, key_up),
            (value_up_h, value_up),
            (query_gain_h, query_gain),
            (query_rotary_h, query_rotary),
            (taps_h, taps),
            (conv_output_h, conv_output),
            (heads_output_h, heads_output),
            (post_gain_h, post_gain),
        ))
    ]
    for load in loads:
        load.start()

    barrier = pltpu.get_barrier_semaphore()

    def greet(dev):
        pl.semaphore_signal(barrier, inc=1, device_id=dev, device_id_type=MESH)

    greet({"z": zup})
    greet({"z": zdown})
    for d in range(1, NP):
        greet(slab_dev(lax.rem(me + d, NP)))
    for d in range(1, NY):
        greet({"y": lax.rem(y + d, NY)})
    far_next = jnp.logical_and(me == NP - 1, z < NZ - 1)
    far_prev = jnp.logical_and(me == 0, z > 0)

    @pl.when(far_next)
    def _():
        greet(next_dev)

    @pl.when(far_prev)
    def _():
        greet(prev_dev)

    pl.semaphore_wait(
        barrier, 2 + NP - 1 + NY - 1 + jnp.where(far_next, 1, 0) + jnp.where(far_prev, 1, 0)
    )

    def up_origin(s):
        return lax.rem(z + NZ - s, NZ)

    def down_origin(s):
        return lax.rem(z + s, NZ)

    def w_copy(origin, column, ssem, dev):
        block = weights.at[origin, column, c]
        return remote(block, block, ssem, w_got.at[column, origin], dev)

    def w_z(way, s):
        origin = up_origin(s) if way == 0 else down_origin(s)
        return w_copy(origin, x, w_sent_z.at[way, s], {"z": zup if way == 0 else zdown})

    def w_x(way, origin):
        return w_copy(origin, x, w_sent_x.at[way, origin], {"x": xright if way == 0 else xleft})

    def w_forward(way, origin):
        column, dev = (xleft, xright) if way == 0 else (xright, xleft)
        return w_copy(origin, column, w_sent_f.at[origin], {"x": dev})

    def w_sibling(origin):
        half = weights.at[origin, :, c]
        return remote(half, half, w_sib_sent.at[origin], w_sib_got.at[origin], {"c": 1 - c})

    def w_wait(column, origin):
        w_copy(origin, column, w_sent_f.at[origin], {"x": xright}).wait_recv()

    def w_start():
        w_z(0, 0).start()
        w_z(1, 0).start()
        w_x(0, z).start()
        w_x(1, z).start()

    def w_step_z(s):
        for way, last in ((0, UP), (1, DOWN)):
            origin = up_origin(s) if way == 0 else down_origin(s)

            @pl.when(s <= last)
            def _():
                w_wait(x, origin)

                @pl.when(s < last)
                def _():
                    w_z(way, s).start()

                w_x(0, origin).start()
                w_x(1, origin).start()

    def w_each(s, act):
        act(up_origin(s))

        @pl.when(jnp.logical_and(s >= 1, s <= DOWN))
        def _():
            act(down_origin(s))

    def w_step_x(s):
        def act(origin):
            w_wait(xleft, origin)
            w_wait(xright, origin)
            even = lax.rem(origin, 2) == 0

            @pl.when(even)
            def _():
                w_forward(0, origin).start()

            @pl.when(jnp.logical_not(even))
            def _():
                w_forward(1, origin).start()

        w_each(s, act)

    def w_step_sibling(s):
        def act(origin):
            w_wait(xfar, origin)
            w_sibling(origin).start()

        w_each(s, act)

    for load in loads[0:3]:
        load.wait()
    w_start()

    for load in loads[3:6]:
        load.wait()
    wide = tokens[...].astype(F32)
    scaled = wide * lax.rsqrt(jnp.mean(wide * wide, axis=-1, keepdims=True) + EPS) * pre_gain[...]
    normed[...] = scaled.astype(BF16)

    latk[y] = dot(normed[...], latent_down[...]).astype(BF16)

    def k_copy(d):
        return remote(latk.at[y], latk.at[y], k_sent.at[d], k_got.at[y], {"y": lax.rem(y + d, NY)})

    def k_arrival(d):
        other = lax.rem(y + d, NY)
        return remote(latk.at[other], latk.at[other], k_sent.at[d], k_got.at[other], {"y": other})

    def q_copy(d):
        return remote(latq.at[y], latq.at[y], q_sent.at[d], q_got.at[y], {"y": lax.rem(y + d, NY)})

    def q_arrival(d):
        other = lax.rem(y + d, NY)
        return remote(latq.at[other], latq.at[other], q_sent.at[d], q_got.at[other], {"y": other})

    for d in range(1, NY):
        k_copy(d).start()
    for load in loads[6:10]:
        load.wait()
    lowered = lax.dot_general(
        down[...], normed[...], (((1,), (1,)), ((), ())), preferred_element_type=F32
    )
    latq[y] = lowered[0:192, :].astype(BF16)
    for d in range(1, NY):
        q_copy(d).start()

    lane = lax.broadcasted_iota(jnp.int32, (ROPE // 2, ROWS), 1)
    mine = lane == z * NP + me

    def far_value(rows):
        return jnp.sum(jnp.where(mine, rows, 0.0), axis=1, keepdims=True)

    cos_near, sin_near = angles[0:16, :], angles[16:32, :]
    cos_far, sin_far = far_value(angles[32:48, :]), far_value(angles[48:64, :])
    cosine = cos_near * cos_far - sin_near * sin_far
    sine = sin_near * cos_far + cos_near * sin_far

    def rotated(turned):
        lead, trail = turned[0:16, :], turned[16:32, :]
        return jnp.concatenate([lead * cosine - trail * sine, trail * cosine + lead * sine], axis=0)

    key_rotary = rotated(lowered[192:224, :]).astype(BF16)
    up_turned[...] = query_up[...].astype(F32).T.astype(BF16)
    for load in loads[10:15]:
        load.wait()
    gain_turned[...] = jnp.broadcast_to(query_gain[...], (ROWS, 768)).T
    w_step_z(jnp.int32(1))

    for d in range(1, NY):
        k_arrival(d).wait_recv()

    latent = jnp.concatenate([latk[i] for i in range(NY)], axis=1).astype(F32)
    latent = latent * lax.rsqrt(jnp.mean(latent * latent, axis=-1, keepdims=True) + EPS)
    latent = (latent * latent_gain[...]).astype(BF16)
    kv[z, 0:128, :] = dot(latent, key_up[...]).astype(BF16)
    kv[z, 128:256, :] = dot(latent, value_up[...]).T.astype(BF16)
    kv[z, 256:288, :] = key_rotary

    def kv_copy(way, s, piece):
        origin = up_origin(s) if way == 0 else down_origin(s)
        rows = kv.at[origin, pl.ds(pl.multiple_of(piece * PIECE, PIECE), PIECE)]
        return remote(
            rows, rows, kv_sent.at[way, s, piece], kv_got.at[origin, piece],
            {"z": zup if way == 0 else zdown},
        )

    def kv_sends(way, s):
        if way == 0:
            return jnp.logical_and(s < UP, jnp.logical_and(z - s >= 0, z < NZ - 1))
        return jnp.logical_and(s < DOWN, down_origin(s) < DOWN)

    def kv_comes(way, s):
        if way == 0:
            return z - s >= 0
        return jnp.logical_and(s <= DOWN, down_origin(s) < DOWN)

    for way in range(2):

        @pl.when(kv_sends(way, 0))
        def _():
            for piece in range(PIECES):
                kv_copy(way, 0, piece).start()

    for d in range(1, NY):
        q_arrival(d).wait_recv()

    parts = [latq[i].astype(F32) for i in range(NY)]
    square = sum(jnp.sum(p * p, axis=0, keepdims=True) for p in parts)
    factor = lax.rsqrt(square * (1.0 / (NY * parts[0].shape[0])) + EPS)
    latent_q = jnp.concatenate(parts, axis=0) * factor * gain_turned[...]
    latent_q = latent_q.astype(BF16)
    queries[me, 0:128, :] = dot(up_turned[...], latent_q).astype(BF16)
    turned = dot(query_rotary[...], latent_q)
    queries[me, 128:160, :] = rotated(turned[0:32, :]).astype(BF16)
    queries[me, 160:192, :] = rotated(turned[32:64, :]).astype(BF16)

    def g_copy(d):
        return remote(
            queries.at[me], queries.at[me], g_sent.at[d], g_got.at[me], slab_dev(lax.rem(me + d, NP))
        )

    def g_arrival(d):
        other = lax.rem(me + d, NP)
        return remote(queries.at[other], queries.at[other], g_sent.at[d], g_got.at[other], slab_dev(other))

    for d in range(1, NP):
        g_copy(d).start()

    w_step_x(jnp.int32(0))
    w_step_z(jnp.int32(2))
    w_step_x(jnp.int32(1))
    w_step_sibling(jnp.int32(0))
    w_step_z(jnp.int32(3))

    acc[...] = jnp.zeros_like(acc)
    stats[0:HEADS, :] = jnp.full((HEADS, SLAB), LOW, F32)
    stats[HEADS : 2 * HEADS, :] = jnp.zeros((HEADS, SLAB), F32)
    for d in range(1, NP):
        g_arrival(d).wait_recv()
    blocks[...] = jnp.zeros_like(blocks)
    for p in range(NP):
        for h in range(HEADS):
            columns = slice(h * SLAB + p * ROWS, h * SLAB + (p + 1) * ROWS)
            blocks[h * NOPE : (h + 1) * NOPE, columns] = queries[p, h * NOPE : (h + 1) * NOPE, :]
            blocks[128:160, columns] = queries[p, 128 + h * ROPE : 128 + (h + 1) * ROPE, :]

    def attend(origin, diagonal):
        keys = kv[origin, 0:128, :]
        rotary = kv[origin, 256:288, :].astype(F32).T.astype(BF16)
        keys = jnp.concatenate([keys, rotary], axis=1)
        for h in range(HEADS):
            values = kv[origin, 128 + h * VDIM : 128 + (h + 1) * VDIM, :]
            for t in range(SLAB // TILE):
                at = slice(t * TILE, (t + 1) * TILE)
                scores = dot(keys, blocks[:, h * SLAB + t * TILE : h * SLAB + (t + 1) * TILE]) * SCALE2
                if diagonal:
                    key = me * ROWS + lax.broadcasted_iota(jnp.int32, (ROWS, TILE), 0)
                    query = t * TILE + lax.broadcasted_iota(jnp.int32, (ROWS, TILE), 1)
                    seen = key <= query
                    scores = jnp.where(seen, scores, LOW)
                old = stats[h : h + 1, at]
                best = jnp.maximum(old, jnp.max(scores, axis=0, keepdims=True))
                weight = jnp.exp2(scores - best)
                if diagonal:
                    weight = jnp.where(seen, weight, 0.0)
                shrink = jnp.exp2(old - best)
                stats[h : h + 1, at] = best
                total = slice(HEADS + h, HEADS + h + 1)
                stats[total, at] = stats[total, at] * shrink + jnp.sum(weight, axis=0, keepdims=True)
                acc[h, :, at] = acc[h, :, at] * shrink + dot(values, weight.astype(BF16))

    attend(z, True)


    def ring_step(s, carry):
        for piece in range(PIECES):
            for way in range(2):

                @pl.when(kv_comes(way, s))
                def _():
                    origin = up_origin(s) if way == 0 else down_origin(s)
                    rows = kv.at[origin, pl.ds(piece * PIECE, PIECE)]
                    remote(
                        rows, rows, kv_sent.at[way, 0, piece], kv_got.at[origin, piece], {"z": zup}
                    ).wait_recv()

                    @pl.when(kv_sends(way, s))
                    def _():
                        kv_copy(way, s, piece).start()

        w_step_z(s + AHEAD)

        @pl.when(s + 1 <= UP)
        def _():
            w_step_x(s + 1)

        w_step_sibling(s)

        @pl.when(z - s >= 0)
        def _():
            attend(up_origin(s), False)

        @pl.when(jnp.logical_and(s <= DOWN, z + s >= NZ))
        def _():
            attend(down_origin(s), False)

        return carry

    lax.fori_loop(1, UP + 1, ring_step, jnp.int32(0))

    for p in range(NP):
        at = slice(p * ROWS, (p + 1) * ROWS)
        for h in range(HEADS):
            sent_o[p, h * VDIM : (h + 1) * VDIM, :] = acc[h, :, at].astype(BF16)
        sent_s[p, 0 : 2 * HEADS, :] = stats[:, at]
        sent_s[p, 2 * HEADS : 8, :] = jnp.zeros((8 - 2 * HEADS, ROWS), F32)

    def o_copy(d):
        p = lax.rem(me + d, NP)
        return remote(sent_o.at[p], got_o.at[me], o_sent.at[d], o_got.at[me], slab_dev(p))

    def s_copy(d):
        p = lax.rem(me + d, NP)
        return remote(sent_s.at[p], got_s.at[me], s_sent.at[d], s_got.at[me], slab_dev(p))

    def o_arrival(d):
        p = lax.rem(me + d, NP)
        return remote(sent_o.at[p], got_o.at[p], o_sent.at[d], o_got.at[p], slab_dev(p))

    def s_arrival(d):
        p = lax.rem(me + d, NP)
        return remote(sent_s.at[p], got_s.at[p], s_sent.at[d], s_got.at[p], slab_dev(p))

    for d in range(1, NP):
        o_copy(d).start()
        s_copy(d).start()
    got_o[me] = sent_o[me]
    got_s[me] = sent_s[me]

    for load in loads[15:19]:
        load.wait()
    mixed_in = None
    for k in range(NZ // 2):
        for i in range(2):
            half = weights.at[2 * k + i, :, 1 - c]
            remote(
                half, half, w_sib_sent.at[2 * k + i], w_sib_got.at[2 * k + i], {"c": 1 - c}
            ).wait_recv()
        part = dot(
            normed[:, 256 * k : 256 * (k + 1)],
            weights[2 * k : 2 * k + 2].reshape(256, 768),
        )
        mixed_in = part if mixed_in is None else mixed_in + part
    outer_part = mixed_in[:, 0:256]
    product[16:144, :] = (mixed_in[:, 256:512] * mixed_in[:, 512:768]).astype(BF16)

    h_copy = remote(product.at[pl.ds(128, 16)], product.at[pl.ds(0, 16)], h_sent, h_got, next_dev)

    @pl.when(has_next)
    def _():
        h_copy.start()

    @pl.when(has_prev)
    def _():
        h_copy.wait_recv()

    @pl.when(jnp.logical_not(has_prev))
    def _():
        product[0:16, :] = jnp.zeros((16, 256), BF16)

    extended = product[...].astype(F32)
    convolved = pltpu.roll(extended, 2, axis=0)[16:144] * taps[0:1, :]
    convolved = convolved + pltpu.roll(extended, 1, axis=0)[16:144] * taps[1:2, :]
    convolved = convolved + extended[16:144] * taps[2:3, :]
    conv_mixed = (outer_part * convolved).astype(BF16)

    for d in range(1, NP):
        o_arrival(d).wait_recv()
        s_arrival(d).wait_recv()

    heads = []
    for h in range(HEADS):
        best = got_s[0, h : h + 1, :]
        for p in range(1, NP):
            best = jnp.maximum(best, got_s[p, h : h + 1, :])
        total, weighted = None, None
        for p in range(NP):
            factor = jnp.exp2(got_s[p, h : h + 1, :] - best)
            a = got_s[p, HEADS + h : HEADS + h + 1, :] * factor
            b = got_o[p, h * VDIM : (h + 1) * VDIM, :].astype(F32) * factor
            total = a if total is None else total + a
            weighted = b if weighted is None else weighted + b
        logsum[h : h + 1, :] = (best + jnp.log2(total)) * (1.0 / LOG2E)
        heads.append(weighted / total)
    heads_mixed = jnp.concatenate(heads, axis=0).T.astype(BF16)

    quarter = ROWS // NY

    def y_copy(d):
        p = lax.rem(y + d, NY)
        return remote(sums.at[p], got_sums.at[y], y_sent.at[d], y_got.at[y], {"y": p})

    def y_arrival(d):
        p = lax.rem(y + d, NY)
        return remote(sums.at[p], got_sums.at[p], y_sent.at[d], y_got.at[p], {"y": p})

    for t in range(4):
        at = slice(t * 512, (t + 1) * 512)
        projected = dot(conv_mixed, conv_output[:, at]) + dot(heads_mixed, heads_output[:, at])
        for p in range(NY):
            sums[p, :, at] = projected[p * quarter : (p + 1) * quarter, :].astype(BF16)
    for d in range(1, NY):
        y_copy(d).start()
    whole = sums[y].astype(F32)
    for d in range(1, NY):
        y_arrival(d).wait_recv()
        whole = whole + got_sums[lax.rem(y + d, NY)].astype(F32)
    whole = whole * lax.rsqrt(jnp.mean(whole * whole, axis=-1, keepdims=True) + EPS) * post_gain[...]
    out[...] = whole.astype(BF16)

    for d in range(1, NY):
        k_copy(d).wait_send()
        q_copy(d).wait_send()
        y_copy(d).wait_send()
    for d in range(1, NP):
        g_copy(d).wait_send()
        o_copy(d).wait_send()
        s_copy(d).wait_send()

    @pl.when(has_next)
    def _():
        h_copy.wait_send()

    def left(s, carry):
        @pl.when(s < UP)
        def _():
            w_z(0, s).wait_send()

        @pl.when(s < DOWN)
        def _():
            w_z(1, s).wait_send()

        w_x(0, s).wait_send()
        w_x(1, s).wait_send()
        w_forward(0, s).wait_send()
        w_sibling(s).wait_send()
        for way in range(2):

            @pl.when(kv_sends(way, s))
            def _():
                for piece in range(PIECES):
                    kv_copy(way, s, piece).wait_send()

        return carry

    lax.fori_loop(0, NZ, left, jnp.int32(0))


def local(
    tokens, pre_gain, outer_gate, inner_gate, conv_input, conv_taps, query_down, latent_down,
    rotary_down, query_gain, latent_gain, query_up, query_rotary, key_up, value_up,
    conv_output, heads_output, post_gain,
):
    width = tokens.shape[1]
    vmem = pl.BlockSpec(memory_space=pltpu.VMEM)
    dma = pltpu.SemaphoreType.DMA
    scratch = [
        pltpu.VMEM((ROWS, width), BF16),
        pltpu.VMEM((1, width), F32),
        pltpu.VMEM((3, 256), F32),
        pltpu.VMEM((224, width), BF16),
        pltpu.VMEM((width, 128), BF16),
        pltpu.VMEM((1, 768), F32),
        pltpu.VMEM((1, 512), F32),
        pltpu.VMEM((768, 128), BF16),
        pltpu.VMEM((64, 768), BF16),
        pltpu.VMEM((512, 128), BF16),
        pltpu.VMEM((512, 128), BF16),
        pltpu.VMEM((256, width), BF16),
        pltpu.VMEM((128, width), BF16),
        pltpu.VMEM((1, width), F32),
        pltpu.VMEM((64, 128), F32),
        pltpu.VMEM((128, 768), BF16),
        pltpu.VMEM((768, 128), F32),
        dma((19,)),
        pltpu.VMEM((ROWS, width), BF16),
        pltpu.VMEM((NZ, NX, NC, 16, 768), BF16),
        pltpu.VMEM((NY, ROWS, 128), BF16),
        pltpu.VMEM((NY, 192, ROWS), BF16),
        pltpu.VMEM((NZ, KV_ROWS, ROWS), BF16),
        pltpu.VMEM((NP, 192, ROWS), BF16),
        pltpu.VMEM((160, HEADS * SLAB), BF16),
        pltpu.VMEM((HEADS, VDIM, SLAB), F32),
        pltpu.VMEM((2 * HEADS, SLAB), F32),
        pltpu.VMEM((NP, HEADS * VDIM, ROWS), BF16),
        pltpu.VMEM((NP, 8, ROWS), F32),
        pltpu.VMEM((NP, HEADS * VDIM, ROWS), BF16),
        pltpu.VMEM((NP, 8, ROWS), F32),
        pltpu.VMEM((16 + ROWS, 256), BF16),
        pltpu.VMEM((NY, ROWS // NY, width), BF16),
        pltpu.VMEM((NY, ROWS // NY, width), BF16),
        dma((NX, NZ)),
        dma((NZ,)),
        dma((2, UP)),
        dma((2, NZ)),
        dma((NZ,)),
        dma((NZ,)),
        dma((NZ, PIECES)),
        dma((2, UP, PIECES)),
        dma((NY,)),
        dma((NY,)),
        dma((NY,)),
        dma((NY,)),
        dma((NP,)),
        dma((NP,)),
        dma((NP,)),
        dma((NP,)),
        dma((NP,)),
        dma((NP,)),
        dma,
        dma,
        dma((NY,)),
        dma((NY,)),
    ]
    return pl.pallas_call(
        kernel,
        out_shape=(
            jax.ShapeDtypeStruct((ROWS // NY, width), BF16),
            jax.ShapeDtypeStruct((HEADS, ROWS), F32),
        ),
        in_specs=[pl.BlockSpec(memory_space=pltpu.HBM)] * 19,
        out_specs=(vmem, vmem),
        scratch_shapes=scratch,
        compiler_params=pltpu.CompilerParams(
            collective_id=0, has_side_effects=True, vmem_limit_bytes=67043328
        ),
        name="layer",
    )(
        tokens, pre_gain.reshape(1, -1), outer_gate, inner_gate, conv_input, conv_taps, query_down.T,
        latent_down, rotary_down.T, query_gain.reshape(1, -1), latent_gain.reshape(1, -1), query_up,
        query_rotary.T, key_up, value_up, conv_output, heads_output, post_gain.reshape(1, -1),
        jnp.asarray(angle_tables()),
    )


def solution(mesh):
    split = Mesh(mesh.devices.reshape(NZ, NX, NC, NY), ("z", "x", "c", "y"))
    return jax.shard_map(
        local,
        mesh=split,
        in_specs=(
            P(SP, None), P(), P(SP, "y"), P(SP, "y"), P(SP, "y"), P(None, "y"), P(None, "y"),
            P(None, "y"), P(), P(), P(), P(None, "y"), P(None, "y"), P(None, "y"), P(None, "y"),
            P("y", None), P("y", None), P(),
        ),
        out_specs=(P(("z", "x", "c", "y"), None), P("y", SP)),
        check_vma=False,
    )
```
